32 devices in a mesh: kv: 4 (over y, x), tp: 8 (over z, core).
Axes of the slice: x: 2, y: 2, z: 4, core: 2. Of those that a mesh axis runs over, the one named last changes fastest.
Arguments:
- tokens: bfloat16 [64, 4096], P('kv', 'tp'), may hold values from -6 to 6
- attn_gain: float32 [4096], replicated, may hold values from 0.1 to 1.9
- w_query: bfloat16 [4096, 2048], P(None, 'tp'), may hold values from -0.09375 to 0.09375
- w_key: bfloat16 [4096, 2048], P(None, 'tp'), may hold values from -0.09375 to 0.09375
- w_value: bfloat16 [4096, 2048], P(None, 'tp'), may hold values from -0.09375 to 0.09375
- w_outgate: bfloat16 [4096, 2048], P(None, 'tp'), may hold values from -0.09375 to 0.09375
- w_rates: bfloat16 [2, 4096, 16], P(None, None, 'tp'), may hold values from -0.09375 to 0.09375
- head_rate: float32 [16], P('tp'), may hold values from 0.02 to 2
- head_gain: float32 [2048], P('tp'), may hold values from 0.1 to 1.9
- w_out: bfloat16 [2048, 4096], P('tp'), may hold values from -0.125 to 0.125
- state: float32 [64, 16, 128, 128], P('kv', 'tp'), may hold values from -2.4 to 2.4
- mlp_gain: float32 [4096], replicated, may hold values from 0.1 to 1.9
- w_gate: bfloat16 [4096, 11264], P(None, ('kv', 'tp')), may hold values from -0.09375 to 0.09375
- w_up: bfloat16 [4096, 11264], P(None, ('kv', 'tp')), may hold values from -0.09375 to 0.09375
- w_down: bfloat16 [4096, 11264], P(None, ('kv', 'tp')), may hold values from -0.109375 to 0.109375
Outputs:
- result: bfloat16 [64, 4096], P('kv', 'tp')
- new_state: float32 [64, 16, 128, 128], P('kv', 'tp')
The draws below stay inside these ranges and needn't reach their ends.
All inputs are finite; a program needn't handle non-finite values.
Results may differ from the reference program's by a relative error of at most 0.014.
Values may be sent and summed in bfloat16 or wider, within the bound.
A program may use at most 64 MiB of HBM per device.

```python
import math
import jax
import jax.numpy as jnp
from jax import lax

D = 4096
H = 16
HEAD = 128
FF = 11264
BATCH = 64


def with_spikes(entries, key, source, target, shards_of, factor):
    owner, partner = [(jnp.arange(entries.shape[axis_at]) // (entries.shape[axis_at] // shards_of)).reshape([-1 if axis == axis_at else 1 for axis in range(entries.ndim)]) for axis_at in (source, target)]
    chosen = jax.random.permutation(key, shards_of)[partner]
    strong = (owner == chosen) | (owner == (partner + shards_of // 2) % shards_of)
    return jnp.where(strong, factor * entries, entries)


def shard_levels(key, shape, cuts, least, top_value):
    level = 1.0
    for axis_at, parts in cuts:
        steps = jax.random.uniform(jax.random.fold_in(jax.random.fold_in(key, 6), axis_at), (parts,), jnp.float32, least / len(cuts), top_value / len(cuts))
        level = level * jnp.repeat(jnp.exp(steps), shape[axis_at] // parts).reshape((-1,) + (1,) * (len(shape) - 1 - axis_at))
    return level


def scatter_about(key, dims, width, reach, shards=(), kind=jnp.bfloat16):
    array = jax.random.normal(key, dims, jnp.float32) * width
    if len(shards) > 0:
        array = shard_levels(key, dims, shards, -0.22, 0.18) * array
    return jnp.clip(array, min=-reach, max=reach).astype(kind)


def heavy_noise(key, dims, width, most, split, heavy, dtype=jnp.bfloat16):
    array = width * jax.random.normal(key, dims, jnp.float32)
    if split:
        array = array * shard_levels(key, dims, split, -0.22, 0.18)
    return jnp.clip(with_spikes(array, jax.random.fold_in(key, 3), *heavy), -most, most).astype(dtype)


def setup_inputs(seed: int = 0) -> dict:
    splits = jax.random.split(jax.random.key(seed), 16)
    return {
        "tokens": scatter_about(splits[0], (BATCH, D), 1.0, 6.0, ((0, 4), (1, 8))),
        "attn_gain": jnp.clip(1.0 + 0.18 * jax.random.normal(splits[1], (D,), jnp.float32), 0.1, 1.9),
        "w_query": scatter_about(splits[2], (D, H * HEAD), D ** -0.5, 0.09375, ((1, 8),)),
        "w_key": scatter_about(splits[3], (D, H * HEAD), D ** -0.5, 0.09375, ((1, 8),)),
        "w_value": scatter_about(splits[4], (D, H * HEAD), D ** -0.5, 0.09375, ((1, 8),)),
        "w_outgate": scatter_about(splits[5], (D, H * HEAD), D ** -0.5, 0.09375, ((1, 8),)),
        "w_rates": scatter_about(splits[6], (2, D, H), D ** -0.5, 0.09375, ((2, 8),)),
        "head_rate": jnp.clip(jnp.exp(math.log(2.0) - 4.6051702 * jax.random.uniform(splits[7], (H,), jnp.float32) ** shard_levels(splits[7], (H,), ((0, 8),), -0.2, 0.2)), 0.02, 2.0),
        "head_gain": jnp.clip(1.0 + 0.18 * jax.random.normal(splits[8], (H * HEAD,), jnp.float32), 0.1, 1.9),
        "w_out": scatter_about(splits[9], (H * HEAD, D), (H * HEAD) ** -0.5, 0.125, ((0, 8),)),
        "state": scatter_about(splits[10], (BATCH, H, HEAD, HEAD), 0.3, 2.4, ((0, 4), (1, 8)), jnp.float32),
        "mlp_gain": jnp.clip(1.0 + 0.18 * jax.random.normal(splits[11], (D,), jnp.float32), 0.1, 1.9),
        "w_gate": scatter_about(splits[12], (D, FF), D ** -0.5, 0.09375, ((1, 32),)),
        "w_up": scatter_about(splits[13], (D, FF), D ** -0.5, 0.09375, ((1, 32),)),
        "w_down": heavy_noise(splits[14], (D, FF), FF ** -0.5, 0.109375, ((1, 32),), (1, 0, 32, 2.75)),
    }


EPS = 1e-06

def row_norm(values, gain):
    floats = values.astype(jnp.float32)
    scaled = floats * lax.rsqrt(lax.optimization_barrier(jnp.mean(floats * floats, axis=-1, keepdims=True)) + EPS)
    return (scaled * gain.astype(jnp.float32)).astype(jnp.bfloat16)

def reference(tokens, attn_gain, w_query, w_key, w_value, w_outgate, w_rates, head_rate, head_gain, w_out, state, mlp_gain, w_gate, w_up, w_down):
    count = tokens.shape[0]
    normed = row_norm(tokens, attn_gain)
    query = jnp.dot(normed, w_query, preferred_element_type=jnp.float32).reshape(count, H, HEAD)
    key = jnp.dot(normed, w_key, preferred_element_type=jnp.float32).reshape(count, H, HEAD)
    value = jnp.dot(normed, w_value, preferred_element_type=jnp.float32).reshape(count, H, HEAD)
    gate_in = jnp.dot(normed, w_outgate, preferred_element_type=jnp.float32).reshape(count, H, HEAD)
    write_raw = jnp.dot(normed, w_rates[0], preferred_element_type=jnp.float32)
    decay_raw = jnp.dot(normed, w_rates[1], preferred_element_type=jnp.float32)
    unit_query = query * lax.rsqrt(lax.optimization_barrier(jnp.sum(query * query, axis=-1, keepdims=True)) + EPS) * HEAD ** (-0.5)
    unit_key = key * lax.rsqrt(lax.optimization_barrier(jnp.sum(key * key, axis=-1, keepdims=True)) + EPS)
    strength = jax.nn.sigmoid(write_raw)
    fade = jnp.exp(-head_rate * jax.nn.softplus(decay_raw))
    carried = state * fade[:, :, None, None]
    fresh = strength[:, :, None] * (value - jnp.einsum('bhi,bhiv->bhv', unit_key, carried))
    new_state = carried + unit_key[:, :, :, None] * fresh[:, :, None, :]
    readout = jnp.einsum('bhi,bhiv->bhv', unit_query, new_state)
    normed_out = readout * lax.rsqrt(lax.optimization_barrier(jnp.mean(readout * readout, axis=-1, keepdims=True)) + EPS)
    mixed = (normed_out * head_gain.reshape(H, HEAD) * jax.nn.silu(gate_in)).astype(jnp.bfloat16).reshape(count, H * HEAD)
    projected = jnp.dot(mixed, w_out, preferred_element_type=jnp.float32)
    residual = (tokens.astype(jnp.float32) + projected).astype(jnp.bfloat16)
    normed_mlp = row_norm(residual, mlp_gain)
    gate_pre = jnp.dot(normed_mlp, w_gate, preferred_element_type=jnp.float32)
    up_pre = jnp.dot(normed_mlp, w_up, preferred_element_type=jnp.float32)
    hidden = (jax.nn.silu(gate_pre) * up_pre).astype(jnp.bfloat16)
    down = lax.dot_general(hidden, w_down, (((1,), (1,)), ((), ())), preferred_element_type=jnp.float32)
    result = (residual.astype(jnp.float32) + down).astype(jnp.bfloat16)
    return (result, new_state)
```

```python
import functools

import jax
import jax.numpy as jnp
from jax import lax
from jax.experimental import pallas as pl
from jax.experimental.pallas import tpu as pltpu
from jax.sharding import PartitionSpec as P

EPS = 1e-06
MESH = pl.DeviceIdType.MESH
NT = (((1,), (1,)), ((), ()))


def remote(src, dst, send_sem, recv_sem, kv, tp):
    return pltpu.make_async_remote_copy(
        src_ref=src,
        dst_ref=dst,
        send_sem=send_sem,
        recv_sem=recv_sem,
        device_id=(kv, tp),
        device_id_type=MESH,
    )


def layer_kernel(
    kv_count,
    tp_count,
    tokens_hbm,
    attn_gain_hbm,
    w_query_hbm,
    w_key_hbm,
    w_value_hbm,
    w_outgate_hbm,
    w_rates_hbm,
    head_rate_ref,
    head_gain_ref,
    w_out_hbm,
    state_hbm,
    mlp_gain_hbm,
    w_gate_hbm,
    w_up_hbm,
    w_down_hbm,
    result_ref,
    new_state_hbm,
    attn_gain,
    w_query,
    w_key,
    w_value,
    w_outgate,
    w_rates,
    w_out,
    state,
    mlp_gain,
    w_gate,
    w_up,
    w_down,
    rows_all,
    share_out,
    share_in,
    res_all,
    pair_out,
    pair_in,
    total,
    group_out,
    group_in,
    last_out,
    last_in,
    load_sem,
    store_sem,
    rows_send,
    rows_recv,
    share_send,
    share_recv,
    res_send_z,
    res_send_kv,
    res_send_pair,
    res_recv,
    pair_send,
    pair_recv,
    group_send,
    group_recv,
    last_send,
    last_recv,
):
    kv = lax.axis_index("kv")
    tp = lax.axis_index("tp")
    z_count = tp_count // 2
    z = tp // 2
    core = tp % 2
    partner = tp + 1 - 2 * core
    count, width = tokens_hbm.shape
    heads = state_hbm.shape[1]
    size = state_hbm.shape[2]
    model = width * tp_count

    def z_peer(step):
        return lax.rem(z + step, z_count)

    def kv_peer(step):
        return lax.rem(kv + step, kv_count)

    own_rows = pltpu.make_async_copy(tokens_hbm, rows_all.at[tp], load_sem.at[0])
    own_rows.start()
    pairs = [
        (attn_gain_hbm, attn_gain),
        (w_rates_hbm, w_rates),
        (w_query_hbm, w_query),
        (w_key_hbm, w_key),
        (w_value_hbm, w_value),
        (w_outgate_hbm, w_outgate),
        (state_hbm, state),
        (w_out_hbm, w_out),
        (mlp_gain_hbm, mlp_gain),
        (w_gate_hbm, w_gate),
        (w_up_hbm, w_up),
        (w_down_hbm, w_down),
    ]
    loads = []
    for index, (source, target) in enumerate(pairs):
        load = pltpu.make_async_copy(source, target, load_sem.at[index + 1])
        load.start()
        loads.append(load)

    barrier = pltpu.get_barrier_semaphore()
    for step in range(1, tp_count):
        pl.semaphore_signal(
            barrier, inc=1, device_id=(kv, lax.rem(tp + step, tp_count)), device_id_type=MESH
        )
    for step in range(1, kv_count):
        pl.semaphore_signal(barrier, inc=1, device_id=(kv_peer(step), tp), device_id_type=MESH)
    pl.semaphore_wait(barrier, tp_count - 1 + kv_count - 1)

    own_rows.wait()
    sent = []
    for step in range(1, tp_count):
        copy = remote(
            rows_all.at[tp],
            rows_all.at[tp],
            rows_send.at[step],
            rows_recv.at[tp],
            kv,
            lax.rem(tp + step, tp_count),
        )
        copy.start()
        sent.append(copy)
    for step in range(1, tp_count):
        source = lax.rem(tp + step, tp_count)
        remote(
            rows_all.at[source],
            rows_all.at[source],
            rows_send.at[step],
            rows_recv.at[source],
            kv,
            source,
        ).wait_recv()

    loads[0].wait()
    loads[1].wait()
    squares = jnp.zeros((count, width), jnp.float32)
    write_sums = [jnp.zeros((count, width), jnp.float32) for _ in range(heads)]
    decay_sums = [jnp.zeros((count, width), jnp.float32) for _ in range(heads)]
    scaled = []
    for block in range(tp_count):
        columns = slice(block * width, (block + 1) * width)
        floats = rows_all[block].astype(jnp.float32)
        squares += floats * floats
        floats = floats * attn_gain[:, columns]
        for head in range(heads):
            write_sums[head] += floats * w_rates[0, head : head + 1, columns].astype(jnp.float32)
            decay_sums[head] += floats * w_rates[1, head : head + 1, columns].astype(jnp.float32)
        scaled.append(floats.astype(jnp.bfloat16))
    norm = lax.rsqrt(jnp.sum(squares, axis=-1, keepdims=True) / model + EPS)

    def project(weight):
        product = jnp.zeros((count, heads * size), jnp.float32)
        for block in range(tp_count):
            product += jnp.dot(
                scaled[block],
                weight[block * width : (block + 1) * width, :],
                preferred_element_type=jnp.float32,
            )
        return product * norm

    loads[2].wait()
    query = project(w_query)
    loads[3].wait()
    key = project(w_key)
    loads[4].wait()
    value = project(w_value)
    loads[5].wait()
    gate_in = project(w_outgate)

    loads[6].wait()
    mixed = []
    for head in range(heads):
        lanes = slice(head * size, (head + 1) * size)
        query_h = query[:, lanes]
        key_h = key[:, lanes]
        unit_query = (
            query_h
            * lax.rsqrt(jnp.sum(query_h * query_h, axis=-1, keepdims=True) + EPS)
            * size ** (-0.5)
        )
        unit_key = key_h * lax.rsqrt(jnp.sum(key_h * key_h, axis=-1, keepdims=True) + EPS)
        write_raw = jnp.sum(write_sums[head], axis=-1, keepdims=True) * norm
        decay_raw = jnp.sum(decay_sums[head], axis=-1, keepdims=True) * norm
        strength = jnp.broadcast_to(jax.nn.sigmoid(write_raw), (count, size))
        rate = head_rate_ref[:, head : head + 1]
        softplus = jnp.maximum(decay_raw, 0.0) + jnp.log1p(jnp.exp(-jnp.abs(decay_raw)))
        fade = jnp.broadcast_to(jnp.exp(-rate * softplus), (count, size))
        query_t = unit_query.T
        key_t = unit_key.T
        rows = []
        for row in range(count):
            here = slice(row, row + 1)
            key_column = key_t[:, here]
            carried = state[row, head] * fade[here, :]
            recalled = jnp.sum(carried * key_column, axis=0, keepdims=True)
            fresh = strength[here, :] * (value[here, lanes] - recalled)
            updated = carried + key_column * fresh
            state[row, head] = updated
            rows.append(jnp.sum(updated * query_t[:, here], axis=0, keepdims=True))
        readout = jnp.concatenate(rows, axis=0)
        normed_out = readout * lax.rsqrt(
            jnp.mean(readout * readout, axis=-1, keepdims=True) + EPS
        )
        gate_h = gate_in[:, lanes]
        silu = gate_h / (1.0 + jnp.exp(-gate_h))
        mixed.append((normed_out * head_gain_ref[:, lanes] * silu).astype(jnp.bfloat16))
    store = pltpu.make_async_copy(state, new_state_hbm, store_sem)
    store.start()

    loads[7].wait()

    def out_block(owner):
        columns = pl.ds(pl.multiple_of(owner * width, width), width)
        product = jnp.zeros((count, width), jnp.float32)
        for head in range(heads):
            product += jnp.dot(
                mixed[head],
                w_out[head * size : (head + 1) * size, columns],
                preferred_element_type=jnp.float32,
            )
        return product

    for step in range(1, tp_count):
        owner = lax.rem(tp + step, tp_count)
        share_out[step] = out_block(owner).astype(jnp.bfloat16)
        copy = remote(
            share_out.at[step],
            share_in.at[tp],
            share_send.at[step],
            share_recv.at[tp],
            kv,
            owner,
        )
        copy.start()
        sent.append(copy)
    residual = rows_all[tp].astype(jnp.float32) + out_block(tp)
    for step in range(1, tp_count):
        source = lax.rem(tp + step, tp_count)
        remote(
            share_out.at[step],
            share_in.at[source],
            share_send.at[step],
            share_recv.at[source],
            kv,
            source,
        ).wait_recv()
        residual += share_in[source].astype(jnp.float32)
    residual = residual.astype(jnp.bfloat16)
    res_all[tp, kv] = residual

    def pass_on(block, group, send_sem, to_kv, to_tp):
        copy = remote(
            res_all.at[block, group],
            res_all.at[block, group],
            send_sem,
            res_recv.at[block, group],
            to_kv,
            to_tp,
        )
        copy.start()
        sent.append(copy)

    def arrival(block, group):
        remote(
            res_all.at[block, group],
            res_all.at[block, group],
            res_send_z.at[0],
            res_recv.at[block, group],
            kv,
            partner,
        ).wait_recv()

    for step in range(1, z_count):
        pass_on(tp, kv, res_send_z.at[step], kv, 2 * z_peer(step) + core)
    for step in range(1, kv_count):
        pass_on(tp, kv, res_send_kv.at[0, step], kv_peer(step), tp)
    pass_on(tp, kv, res_send_pair.at[0, 0], kv, partner)
    for z_step in range(1, z_count):
        block = 2 * z_peer(z_step) + core
        arrival(block, kv)
        for step in range(1, kv_count):
            pass_on(block, kv, res_send_kv.at[z_step, step], kv_peer(step), tp)
        pass_on(block, kv, res_send_pair.at[z_step, 0], kv, partner)
    for z_step in range(z_count):
        block = 2 * z_peer(z_step) + core
        for step in range(1, kv_count):
            arrival(block, kv_peer(step))
            pass_on(block, kv_peer(step), res_send_pair.at[z_step, step], kv, partner)
    for z_step in range(z_count):
        block = 2 * z_peer(z_step) + 1 - core
        for step in range(kv_count):
            arrival(block, kv_peer(step))

    everyone = kv_count * count
    units = w_gate_hbm.shape[0]
    for index in (8, 9, 10):
        loads[index].wait()
    squares = jnp.zeros((everyone, width), jnp.float32)
    gate_pre = jnp.zeros((everyone, units), jnp.float32)
    up_pre = jnp.zeros((everyone, units), jnp.float32)
    for block in range(tp_count):
        columns = slice(block * width, (block + 1) * width)
        floats = res_all[block].reshape(everyone, width).astype(jnp.float32)
        squares += floats * floats
        part = (floats * mlp_gain[:, columns]).astype(jnp.bfloat16)
        gate_pre += lax.dot_general(
            part, w_gate[:, columns], NT, preferred_element_type=jnp.float32
        )
        up_pre += lax.dot_general(part, w_up[:, columns], NT, preferred_element_type=jnp.float32)
    norm = lax.rsqrt(jnp.sum(squares, axis=-1, keepdims=True) / model + EPS)
    gate_pre = gate_pre * norm
    hidden = (gate_pre / (1.0 + jnp.exp(-gate_pre)) * (up_pre * norm)).astype(jnp.bfloat16)
    loads[11].wait()

    def down_block(owner):
        columns = pl.ds(pl.multiple_of(owner * width, width), width)
        product = jnp.dot(hidden, w_down[:, columns], preferred_element_type=jnp.float32)
        return product.reshape(kv_count, count, width)

    for step in range(z_count):
        there = z_peer(step)
        pair_out[step] = down_block(2 * there + 1 - core).astype(jnp.bfloat16)
        copy = remote(
            pair_out.at[step],
            pair_in.at[there],
            pair_send.at[step],
            pair_recv.at[there],
            kv,
            partner,
        )
        copy.start()
        sent.append(copy)
    for step in range(z_count):
        there = z_peer(step)
        total[there] = down_block(2 * there + core)
    order = [step for step in range(1, z_count)] + [0]
    for step in order:
        there = z_peer(step)
        remote(
            pair_out.at[step],
            pair_in.at[there],
            pair_send.at[step],
            pair_recv.at[there],
            kv,
            partner,
        ).wait_recv()
        for kv_step in range(1, kv_count):
            group = kv_peer(kv_step)
            both = total[there, group] + pair_in[there, group].astype(jnp.float32)
            group_out[there, group] = both.astype(jnp.bfloat16)
            copy = remote(
                group_out.at[there, group],
                group_in.at[there, kv],
                group_send.at[step, kv_step],
                group_recv.at[there, kv],
                group,
                tp,
            )
            copy.start()
            sent.append(copy)
    mine = None
    for step in order:
        there = z_peer(step)
        both = total[there, kv] + pair_in[there, kv].astype(jnp.float32)
        for kv_step in range(1, kv_count):
            group = kv_peer(kv_step)
            remote(
                group_out.at[there, group],
                group_in.at[there, group],
                group_send.at[step, kv_step],
                group_recv.at[there, group],
                group,
                tp,
            ).wait_recv()
            both += group_in[there, group].astype(jnp.float32)
        if step == 0:
            mine = both
            continue
        last_out[step] = both.astype(jnp.bfloat16)
        copy = remote(
            last_out.at[step],
            last_in.at[z],
            last_send.at[step],
            last_recv.at[z],
            kv,
            2 * there + core,
        )
        copy.start()
        sent.append(copy)
    mine += residual.astype(jnp.float32)
    for step in range(1, z_count):
        there = z_peer(step)
        remote(
            last_out.at[step],
            last_in.at[there],
            last_send.at[step],
            last_recv.at[there],
            kv,
            2 * there + core,
        ).wait_recv()
        mine += last_in[there].astype(jnp.float32)
    result_ref[...] = mine.astype(jnp.bfloat16)

    for copy in sent:
        copy.wait_send()
    store.wait()


def body(
    kv_count,
    tp_count,
    tokens,
    attn_gain,
    w_query,
    w_key,
    w_value,
    w_outgate,
    w_rates,
    head_rate,
    head_gain,
    w_out,
    state,
    mlp_gain,
    w_gate,
    w_up,
    w_down,
):
    count, width = tokens.shape
    heads = head_rate.shape[0]
    z_count = tp_count // 2
    operands = (
        tokens,
        attn_gain.reshape(1, -1),
        w_query,
        w_key,
        w_value,
        w_outgate,
        w_rates.transpose(0, 2, 1),
        head_rate.reshape(1, -1),
        head_gain.reshape(1, -1),
        w_out,
        state,
        mlp_gain.reshape(1, -1),
        w_gate.T,
        w_up.T,
        w_down.T,
    )
    in_vmem = (7, 8)
    anywhere = pl.BlockSpec(memory_space=pl.ANY)
    vmem = pl.BlockSpec(memory_space=pltpu.VMEM)
    local = [
        pltpu.VMEM(operands[index].shape, operands[index].dtype)
        for index in (1, 2, 3, 4, 5, 6, 9, 10, 11, 12, 13, 14)
    ]
    bf16 = jnp.bfloat16
    dma = pltpu.SemaphoreType.DMA
    exchange = [
        pltpu.VMEM((tp_count, count, width), bf16),
        pltpu.VMEM((tp_count, count, width), bf16),
        pltpu.VMEM((tp_count, count, width), bf16),
        pltpu.VMEM((tp_count, kv_count, count, width), bf16),
        pltpu.VMEM((z_count, kv_count, count, width), bf16),
        pltpu.VMEM((z_count, kv_count, count, width), bf16),
        pltpu.VMEM((z_count, kv_count, count, width), jnp.float32),
        pltpu.VMEM((z_count, kv_count, count, width), bf16),
        pltpu.VMEM((z_count, kv_count, count, width), bf16),
        pltpu.VMEM((z_count, count, width), bf16),
        pltpu.VMEM((z_count, count, width), bf16),
        dma((len(local) + 1,)),
        dma,
        dma((tp_count,)),
        dma((tp_count,)),
        dma((tp_count,)),
        dma((tp_count,)),
        dma((z_count,)),
        dma((z_count, kv_count)),
        dma((z_count, kv_count)),
        dma((tp_count, kv_count)),
        dma((z_count,)),
        dma((z_count,)),
        dma((z_count, kv_count)),
        dma((z_count, kv_count)),
        dma((z_count,)),
        dma((z_count,)),
    ]
    return pl.pallas_call(
        functools.partial(layer_kernel, kv_count, tp_count),
        out_shape=(
            jax.ShapeDtypeStruct(tokens.shape, bf16),
            jax.ShapeDtypeStruct(state.shape, jnp.float32),
        ),
        in_specs=[vmem if index in in_vmem else anywhere for index in range(len(operands))],
        out_specs=(vmem, anywhere),
        scratch_shapes=local + exchange,
        compiler_params=pltpu.CompilerParams(
            collective_id=0, has_side_effects=True, vmem_limit_bytes=60 * 1024 * 1024
        ),
        name="layer",
    )(*operands)


def solution(mesh):
    return jax.shard_map(
        functools.partial(body, mesh.shape["kv"], mesh.shape["tp"]),
        mesh=mesh,
        in_specs=(
            P("kv", "tp"),
            P(),
            P(None, "tp"),
            P(None, "tp"),
            P(None, "tp"),
            P(None, "tp"),
            P(None, None, "tp"),
            P("tp"),
            P("tp"),
            P("tp", None),
            P("kv", "tp", None, None),
            P(),
            P(None, ("kv", "tp")),
            P(None, ("kv", "tp")),
            P(None, ("kv", "tp")),
        ),
        out_specs=(P("kv", "tp"), P("kv", "tp", None, None)),
        check_vma=False,
    )
```

```python
import functools

import jax
import jax.numpy as jnp
from jax import lax
from jax.experimental import pallas as pl
from jax.experimental.pallas import tpu as pltpu
from jax.sharding import PartitionSpec as P

EPS = 1e-06
MESH = pl.DeviceIdType.MESH
NT = (((1,), (1,)), ((), ()))


def remote(src, dst, send_sem, recv_sem, kv, tp):
    return pltpu.make_async_remote_copy(
        src_ref=src,
        dst_ref=dst,
        send_sem=send_sem,
        recv_sem=recv_sem,
        device_id=(kv, tp),
        device_id_type=MESH,
    )


def paired(index, step, count):
    if count & (count - 1):
        return lax.rem(index + step, count)
    bit = 1
    while bit < count:
        if step & bit:
            index = index + bit - 2 * bit * ((index // bit) % 2)
        bit *= 2
    return index


def layer_kernel(
    kv_count,
    tp_count,
    tokens_hbm,
    attn_gain_hbm,
    w_query_hbm,
    w_key_hbm,
    w_value_hbm,
    w_outgate_hbm,
    w_rates_hbm,
    head_rate_ref,
    head_gain_ref,
    w_out_hbm,
    state_hbm,
    mlp_gain_hbm,
    w_gate_hbm,
    w_up_hbm,
    w_down_hbm,
    result_ref,
    new_state,
    attn_gain,
    w_query,
    w_key,
    w_value,
    w_outgate,
    w_rates,
    w_out,
    state,
    mlp_gain,
    w_gate,
    w_up,
    w_down,
    rows_all,
    share_out,
    share_in,
    res_all,
    pair_out,
    pair_in,
    total,
    group_out,
    group_in,
    last_out,
    last_in,
    load_sem,
    rows_send,
    rows_recv,
    share_send,
    share_recv,
    res_send_z,
    res_send_kv,
    res_send_pair,
    res_recv,
    pair_send,
    pair_recv,
    group_send,
    group_recv,
    last_send,
    last_recv,
):
    kv = lax.axis_index("kv")
    tp = lax.axis_index("tp")
    z_count = tp_count // 2
    z = tp // 2
    core = tp % 2
    partner = tp + 1 - 2 * core
    count, width = tokens_hbm.shape
    heads = state_hbm.shape[1]
    size = state_hbm.shape[2]
    model = width * tp_count

    def z_peer(step):
        return paired(z, step, z_count)

    def kv_peer(step):
        return paired(kv, step, kv_count)

    def tp_peer(step):
        return paired(tp, step, tp_count)

    own_rows = pltpu.make_async_copy(tokens_hbm, rows_all.at[tp], load_sem.at[0])
    own_rows.start()
    pairs = [
        (attn_gain_hbm, attn_gain),
        (w_rates_hbm, w_rates),
        (w_query_hbm, w_query),
        (w_key_hbm, w_key),
        (w_value_hbm, w_value),
        (w_outgate_hbm, w_outgate),
        (state_hbm, state),
        (w_out_hbm, w_out),
        (mlp_gain_hbm, mlp_gain),
        (w_gate_hbm, w_gate),
        (w_up_hbm, w_up),
        (w_down_hbm, w_down),
    ]
    loads = []
    for index, (source, target) in enumerate(pairs):
        load = pltpu.make_async_copy(source, target, load_sem.at[index + 1])
        load.start()
        loads.append(load)

    barrier = pltpu.get_barrier_semaphore()
    for step in range(1, tp_count):
        pl.semaphore_signal(
            barrier, inc=1, device_id=(kv, tp_peer(step)), device_id_type=MESH
        )
    for step in range(1, kv_count):
        pl.semaphore_signal(barrier, inc=1, device_id=(kv_peer(step), tp), device_id_type=MESH)
    pl.semaphore_wait(barrier, tp_count - 1 + kv_count - 1)

    own_rows.wait()
    sent = []
    for step in range(tp_count - 1, 0, -1):
        copy = remote(
            rows_all.at[tp],
            rows_all.at[tp],
            rows_send.at[step],
            rows_recv.at[tp],
            kv,
            tp_peer(step),
        )
        copy.start()
        sent.append(copy)
    loads[0].wait()
    loads[1].wait()
    squares = jnp.zeros((count, width), jnp.float32)
    write_sums = [jnp.zeros((count, width), jnp.float32) for _ in range(heads)]
    decay_sums = [jnp.zeros((count, width), jnp.float32) for _ in range(heads)]
    sums = [jnp.zeros((count, heads * size), jnp.float32) for _ in range(4)]
    for step in range(tp_count):
        source = tp_peer(step)
        if step > 0:
            remote(
                rows_all.at[source],
                rows_all.at[source],
                rows_send.at[step],
                rows_recv.at[source],
                kv,
                source,
            ).wait_recv()
        here = pl.ds(pl.multiple_of(source * width, width), width)
        floats = rows_all[source].astype(jnp.float32)
        squares += floats * floats
        floats = floats * attn_gain[:, here]
        for head in range(heads):
            write_sums[head] += floats * w_rates[0, head : head + 1, here].astype(jnp.float32)
            decay_sums[head] += floats * w_rates[1, head : head + 1, here].astype(jnp.float32)
        scaled = floats.astype(jnp.bfloat16)
        for index, weight in enumerate((w_query, w_key, w_value, w_outgate)):
            if step == 0:
                loads[2 + index].wait()
            sums[index] += jnp.dot(scaled, weight[here, :], preferred_element_type=jnp.float32)
    norm = lax.rsqrt(jnp.sum(squares, axis=-1, keepdims=True) / model + EPS)
    query, key, value, gate_in = [part * norm for part in sums]

    loads[6].wait()
    mixed = []
    for head in range(heads):
        lanes = slice(head * size, (head + 1) * size)
        query_h = query[:, lanes]
        key_h = key[:, lanes]
        unit_query = (
            query_h
            * lax.rsqrt(jnp.sum(query_h * query_h, axis=-1, keepdims=True) + EPS)
            * size ** (-0.5)
        )
        unit_key = key_h * lax.rsqrt(jnp.sum(key_h * key_h, axis=-1, keepdims=True) + EPS)
        write_raw = jnp.sum(write_sums[head], axis=-1, keepdims=True) * norm
        decay_raw = jnp.sum(decay_sums[head], axis=-1, keepdims=True) * norm
        strength = jnp.broadcast_to(jax.nn.sigmoid(write_raw), (count, size))
        rate = head_rate_ref[:, head : head + 1]
        softplus = jnp.maximum(decay_raw, 0.0) + jnp.log1p(jnp.exp(-jnp.abs(decay_raw)))
        fade = jnp.broadcast_to(jnp.exp(-rate * softplus), (count, size))
        query_t = unit_query.T
        key_t = unit_key.T
        rows = []
        for row in range(count):
            here = slice(row, row + 1)
            key_column = key_t[:, here]
            carried = state[row, head] * fade[here, :]
            recalled = jnp.sum(carried * key_column, axis=0, keepdims=True)
            fresh = strength[here, :] * (value[here, lanes] - recalled)
            updated = carried + key_column * fresh
            new_state[row, head] = updated
            rows.append(jnp.sum(updated * query_t[:, here], axis=0, keepdims=True))
        readout = jnp.concatenate(rows, axis=0)
        normed_out = readout * lax.rsqrt(
            jnp.mean(readout * readout, axis=-1, keepdims=True) + EPS
        )
        gate_h = gate_in[:, lanes]
        silu = gate_h / (1.0 + jnp.exp(-gate_h))
        mixed.append((normed_out * head_gain_ref[:, lanes] * silu).astype(jnp.bfloat16))

    loads[7].wait()

    def out_block(owner):
        columns = pl.ds(pl.multiple_of(owner * width, width), width)
        product = jnp.zeros((count, width), jnp.float32)
        for head in range(heads):
            product += jnp.dot(
                mixed[head],
                w_out[head * size : (head + 1) * size, columns],
                preferred_element_type=jnp.float32,
            )
        return product

    for step in range(tp_count - 1, 0, -1):
        owner = tp_peer(step)
        share_out[step] = out_block(owner).astype(jnp.bfloat16)
        copy = remote(
            share_out.at[step],
            share_in.at[tp],
            share_send.at[step],
            share_recv.at[tp],
            kv,
            owner,
        )
        copy.start()
        sent.append(copy)
    residual = rows_all[tp].astype(jnp.float32) + out_block(tp)
    for step in range(1, tp_count):
        source = tp_peer(step)
        remote(
            share_out.at[step],
            share_in.at[source],
            share_send.at[step],
            share_recv.at[source],
            kv,
            source,
        ).wait_recv()
        residual += share_in[source].astype(jnp.float32)
    residual = residual.astype(jnp.bfloat16)
    res_all[tp, kv] = residual

    def pass_on(block, group, send_sem, to_kv, to_tp):
        copy = remote(
            res_all.at[block, group],
            res_all.at[block, group],
            send_sem,
            res_recv.at[block, group],
            to_kv,
            to_tp,
        )
        copy.start()
        sent.append(copy)

    def arrival(block, group):
        remote(
            res_all.at[block, group],
            res_all.at[block, group],
            res_send_z.at[0],
            res_recv.at[block, group],
            kv,
            partner,
        ).wait_recv()

    for step in range(z_count - 1, 0, -1):
        pass_on(tp, kv, res_send_z.at[step], kv, 2 * z_peer(step) + core)
    for step in range(kv_count - 1, 0, -1):
        pass_on(tp, kv, res_send_kv.at[0, step], kv_peer(step), tp)
    pass_on(tp, kv, res_send_pair.at[0, 0], kv, partner)
    for z_step in range(1, z_count):
        block = 2 * z_peer(z_step) + core
        arrival(block, kv)
        for step in range(kv_count - 1, 0, -1):
            pass_on(block, kv, res_send_kv.at[z_step, step], kv_peer(step), tp)
        pass_on(block, kv, res_send_pair.at[z_step, 0], kv, partner)
    for z_step in range(z_count):
        block = 2 * z_peer(z_step) + core
        for step in range(1, kv_count):
            arrival(block, kv_peer(step))
            pass_on(block, kv_peer(step), res_send_pair.at[z_step, step], kv, partner)

    everyone = kv_count * count
    units = w_gate_hbm.shape[0]
    for index in (8, 9, 10):
        loads[index].wait()
    squares = jnp.zeros((everyone, width), jnp.float32)
    gate_pre = jnp.zeros((everyone, units), jnp.float32)
    up_pre = jnp.zeros((everyone, units), jnp.float32)
    for side in range(2):
        for z_step in range(z_count):
            block = 2 * z_peer(z_step) + core + side * (1 - 2 * core)
            if side == 1:
                for step in range(kv_count):
                    arrival(block, kv_peer(step))
            here = pl.ds(pl.multiple_of(block * width, width), width)
            floats = res_all[block].reshape(everyone, width).astype(jnp.float32)
            squares += floats * floats
            part = (floats * mlp_gain[:, here]).astype(jnp.bfloat16)
            gate_pre += lax.dot_general(
                part, w_gate[:, here], NT, preferred_element_type=jnp.float32
            )
            up_pre += lax.dot_general(part, w_up[:, here], NT, preferred_element_type=jnp.float32)
    norm = lax.rsqrt(jnp.sum(squares, axis=-1, keepdims=True) / model + EPS)
    gate_pre = gate_pre * norm
    hidden = (gate_pre / (1.0 + jnp.exp(-gate_pre)) * (up_pre * norm)).astype(jnp.bfloat16)
    loads[11].wait()

    def down_block(owner):
        columns = pl.ds(pl.multiple_of(owner * width, width), width)
        product = jnp.dot(hidden, w_down[:, columns], preferred_element_type=jnp.float32)
        return product.reshape(kv_count, count, width)

    order = list(range(z_count - 1, -1, -1))
    for step in order:
        there = z_peer(step)
        pair_out[step] = down_block(2 * there + 1 - core).astype(jnp.bfloat16)
        copy = remote(
            pair_out.at[step],
            pair_in.at[there],
            pair_send.at[step],
            pair_recv.at[there],
            kv,
            partner,
        )
        copy.start()
        sent.append(copy)
    for step in order:
        there = z_peer(step)
        total[there] = down_block(2 * there + core)
    for step in order:
        there = z_peer(step)
        remote(
            pair_out.at[step],
            pair_in.at[there],
            pair_send.at[step],
            pair_recv.at[there],
            kv,
            partner,
        ).wait_recv()
        for kv_step in range(kv_count - 1, 0, -1):
            group = kv_peer(kv_step)
            both = total[there, group] + pair_in[there, group].astype(jnp.float32)
            group_out[there, group] = both.astype(jnp.bfloat16)
            copy = remote(
                group_out.at[there, group],
                group_in.at[there, kv],
                group_send.at[step, kv_step],
                group_recv.at[there, kv],
                group,
                tp,
            )
            copy.start()
            sent.append(copy)
    mine = None
    for step in order:
        there = z_peer(step)
        both = total[there, kv] + pair_in[there, kv].astype(jnp.float32)
        for kv_step in range(1, kv_count):
            group = kv_peer(kv_step)
            remote(
                group_out.at[there, group],
                group_in.at[there, group],
                group_send.at[step, kv_step],
                group_recv.at[there, group],
                group,
                tp,
            ).wait_recv()
            both += group_in[there, group].astype(jnp.float32)
        if step == 0:
            mine = both
            continue
        last_out[step] = both.astype(jnp.bfloat16)
        copy = remote(
            last_out.at[step],
            last_in.at[z],
            last_send.at[step],
            last_recv.at[z],
            kv,
            2 * there + core,
        )
        copy.start()
        sent.append(copy)
    mine += residual.astype(jnp.float32)
    for step in range(1, z_count):
        there = z_peer(step)
        remote(
            last_out.at[step],
            last_in.at[there],
            last_send.at[step],
            last_recv.at[there],
            kv,
            2 * there + core,
        ).wait_recv()
        mine += last_in[there].astype(jnp.float32)
    result_ref[...] = mine.astype(jnp.bfloat16)

    for copy in sent:
        copy.wait_send()


def body(
    kv_count,
    tp_count,
    tokens,
    attn_gain,
    w_query,
    w_key,
    w_value,
    w_outgate,
    w_rates,
    head_rate,
    head_gain,
    w_out,
    state,
    mlp_gain,
    w_gate,
    w_up,
    w_down,
):
    count, width = tokens.shape
    heads = head_rate.shape[0]
    z_count = tp_count // 2
    operands = (
        tokens,
        attn_gain.reshape(1, -1),
        w_query,
        w_key,
        w_value,
        w_outgate,
        w_rates.transpose(0, 2, 1),
        head_rate.reshape(1, -1),
        head_gain.reshape(1, -1),
        w_out,
        state,
        mlp_gain.reshape(1, -1),
        w_gate.T,
        w_up.T,
        w_down.T,
    )
    in_vmem = (7, 8)
    anywhere = pl.BlockSpec(memory_space=pl.ANY)
    vmem = pl.BlockSpec(memory_space=pltpu.VMEM)
    local = [
        pltpu.VMEM(operands[index].shape, operands[index].dtype)
        for index in (1, 2, 3, 4, 5, 6, 9, 10, 11, 12, 13, 14)
    ]
    bf16 = jnp.bfloat16
    dma = pltpu.SemaphoreType.DMA
    exchange = [
        pltpu.VMEM((tp_count, count, width), bf16),
        pltpu.VMEM((tp_count, count, width), bf16),
        pltpu.VMEM((tp_count, count, width), bf16),
        pltpu.VMEM((tp_count, kv_count, count, width), bf16),
        pltpu.VMEM((z_count, kv_count, count, width), bf16),
        pltpu.VMEM((z_count, kv_count, count, width), bf16),
        pltpu.VMEM((z_count, kv_count, count, width), jnp.float32),
        pltpu.VMEM((z_count, kv_count, count, width), bf16),
        pltpu.VMEM((z_count, kv_count, count, width), bf16),
        pltpu.VMEM((z_count, count, width), bf16),
        pltpu.VMEM((z_count, count, width), bf16),
        dma((len(local) + 1,)),
        dma((tp_count,)),
        dma((tp_count,)),
        dma((tp_count,)),
        dma((tp_count,)),
        dma((z_count,)),
        dma((z_count, kv_count)),
        dma((z_count, kv_count)),
        dma((tp_count, kv_count)),
        dma((z_count,)),
        dma((z_count,)),
        dma((z_count, kv_count)),
        dma((z_count, kv_count)),
        dma((z_count,)),
        dma((z_count,)),
    ]
    return pl.pallas_call(
        functools.partial(layer_kernel, kv_count, tp_count),
        out_shape=(
            pltpu.VMEM(tokens.shape, bf16),
            pltpu.VMEM(state.shape, jnp.float32),
        ),
        in_specs=[vmem if index in in_vmem else anywhere for index in range(len(operands))],
        out_specs=(vmem, vmem),
        scratch_shapes=local + exchange,
        compiler_params=pltpu.CompilerParams(
            collective_id=0, has_side_effects=True, vmem_limit_bytes=60 * 1024 * 1024
        ),
        name="layer",
    )(*operands)


def solution(mesh):
    return jax.shard_map(
        functools.partial(body, mesh.shape["kv"], mesh.shape["tp"]),
        mesh=mesh,
        in_specs=(
            P("kv", "tp"),
            P(),
            P(None, "tp"),
            P(None, "tp"),
            P(None, "tp"),
            P(None, "tp"),
            P(None, None, "tp"),
            P("tp"),
            P("tp"),
            P("tp", None),
            P("kv", "tp", None, None),
            P(),
            P(None, ("kv", "tp")),
            P(None, ("kv", "tp")),
            P(None, ("kv", "tp")),
        ),
        out_specs=(P("kv", "tp"), P("kv", "tp", None, None)),
        check_vma=False,
    )
```
